32 devices in a mesh: ep: 8 (over z, core), tp: 4 (over y, x).
Axes of the slice: x: 2, y: 2, z: 4, core: 2. Of those that a mesh axis runs over, the one named last changes fastest.
Arguments:
- queries: bfloat16 [2048, 2048], P('ep', 'tp'), may hold values from -6 to 6
- keys: bfloat16 [2048, 2048], P('ep', 'tp'), may hold values from -6 to 6
- values: bfloat16 [2048, 2048], P('ep', 'tp'), may hold values from -6 to 6
- gates: bfloat16 [2048, 2048], P('ep', 'tp'), may hold values from -6 to 6
- log_decay: float32 [2048, 16], P('ep', 'tp'), may hold values from -2 to 0
- out_weight: bfloat16 [2048, 2048], P(None, 'tp'), may hold values from -0.125 to 0.125
- moe_rows: bfloat16 [2048, 2048], P('ep'), may hold values from -140 to 140
- moe_gain: bfloat16 [2048], replicated, may hold values from 0.099609375 to 1.8984375
- routes: int32 [2048, 2], P('ep'), may hold values from 0 to 7, as said below
- route_weights: float32 [2048, 2], P('ep'), may hold values from 0.1 to 1
- gate_proj: bfloat16 [8, 2048, 4096], P('ep', None, 'tp'), may hold values from -0.125 to 0.125
- up_proj: bfloat16 [8, 2048, 4096], P('ep', None, 'tp'), may hold values from -0.125 to 0.125
- down_proj: bfloat16 [8, 4096, 2048], P('ep', None, 'tp'), may hold values from -0.09375 to 0.09375
Outputs:
- mixer_out: bfloat16 [2048, 2048], P('ep', 'tp')
- moe_out: bfloat16 [2048, 2048], P('ep', 'tp')
The draws below stay inside these ranges and needn't reach their ends.
Inputs may be any that keep to these rules, and one draw needn't show every extreme that they name: `routes`: each row names two different experts of one group of 8 consecutive experts; in each aligned block of 256 rows every expert is named by exactly 64 rows.
All inputs are finite; a program needn't handle non-finite values.
Results may differ from the reference program's by a relative error of at most 0.011.
Values may be sent and summed in bfloat16 or wider, within the bound.
A program may use at most 64 MiB of HBM per device.

```python
import math
import jax
import jax.numpy as jnp
from jax import lax

D = 2048
RETENTION_HEADS = 16
HEAD_DIM = 128
FF = 4096
EXP_GROUP = 8
BLOCK = 128
ROWS_MIX = 256
ROWS_MOE = 256
MIXER_TOKENS = 2048
TOKENS_MOE = 2048
EXPERTS = 8
GROUPS = 1


def draw_log_decay(key, part):
    k_fast = jax.random.fold_in(key, 11)
    k_rate = jax.random.fold_in(key, 12)
    k_slow = jax.random.fold_in(key, 13)
    k_block = jax.random.fold_in(key, 14)
    k_rough = jax.random.fold_in(key, 15)
    location_random_key = jax.random.fold_in(key, 16)
    spike_random_key = jax.random.fold_in(key, 17)
    fast_share = 0.5
    is_fast = jax.random.uniform(k_fast, (RETENTION_HEADS,)) < fast_share
    fast_rate = jax.random.uniform(k_rate, (RETENTION_HEADS,), minval=2.5, maxval=4.0) / BLOCK
    slow_rate = jax.random.uniform(k_slow, (RETENTION_HEADS,), minval=0.1, maxval=0.35) / MIXER_TOKENS
    baseline_decay_rate = jnp.where(is_fast, fast_rate, slow_rate)
    span_count = MIXER_TOKENS // ROWS_MIX
    extent_multiplier = jnp.exp(jax.random.uniform(k_block, (span_count, RETENTION_HEADS), minval=-math.log(2.0), maxval=math.log(2.0)))
    extent_multiplier = jnp.repeat(extent_multiplier, ROWS_MIX, axis=0)
    jitter_multiplier = jnp.exp(jax.random.uniform(k_rough, (MIXER_TOKENS, RETENTION_HEADS), minval=-0.7, maxval=0.7))
    spike_locations = jax.random.randint(location_random_key, (2, RETENTION_HEADS), 0, MIXER_TOKENS)
    spike_strength = jnp.log(jax.random.uniform(spike_random_key, (2, RETENTION_HEADS), minval=0.5, maxval=0.8))
    token_place = jnp.arange(MIXER_TOKENS, dtype=jnp.int32)[None, :, None]
    decay_spikes = jnp.sum(jnp.where(token_place == spike_locations[:, None, :], spike_strength[:, None, :], 0.0), axis=0)
    return (decay_spikes - baseline_decay_rate[None, :] * extent_multiplier * jitter_multiplier).astype(jnp.float32)


def draw_moe_rows(key, part):
    k_base = jax.random.fold_in(key, 21)
    k_column = jax.random.fold_in(key, 22)
    base = jax.random.truncated_normal(k_base, -4.0, 4.0, (TOKENS_MOE, D))
    column_scale = jnp.exp(jax.random.uniform(k_column, (D,), minval=0.0, maxval=math.log(10.0)))
    result = base * column_scale[None, :]
    return result.astype(jnp.bfloat16)


def draw_routes(key, part):
    k_perm = jax.random.fold_in(key, 31)
    k_first = jax.random.fold_in(key, 32)
    k_second = jax.random.fold_in(key, 33)
    span_count = TOKENS_MOE // ROWS_MOE
    orders = jax.vmap(lambda single: jax.random.permutation(single, ROWS_MOE))(jax.random.split(k_perm, span_count))
    ranked = jnp.argsort(orders, axis=1, stable=True).astype(jnp.int32)
    group_id = ranked % GROUPS
    local_rank = ranked // GROUPS
    first_offset = jax.random.randint(k_first, (span_count, GROUPS), 0, EXP_GROUP)
    second_offset = jax.random.randint(k_second, (span_count, GROUPS), 0, EXP_GROUP - 1)
    first_pick = (local_rank + jnp.take_along_axis(first_offset, group_id, axis=1)) % EXP_GROUP
    second_step = (local_rank // EXP_GROUP + jnp.take_along_axis(second_offset, group_id, axis=1)) % (EXP_GROUP - 1)
    second_pick = (first_pick + 1 + second_step) % EXP_GROUP
    chosen = jnp.stack([group_id * EXP_GROUP + first_pick, group_id * EXP_GROUP + second_pick], axis=-1)
    return chosen.reshape(TOKENS_MOE, 2).astype(jnp.int32)


def block_levels(stream_key, dims, cuts, least, high):
    def one(dim, shards_of):
        draws = jax.random.uniform(jax.random.fold_in(jax.random.fold_in(stream_key, 6), dim), (shards_of,), jnp.float32, least / len(cuts), high / len(cuts))
        return jnp.repeat(jnp.exp(draws), dims[dim] // shards_of).reshape((-1,) + (1,) * (len(dims) - dim - 1))

    gain = one(*cuts[0])
    for cut in cuts[1:]:
        gain = gain * one(*cut)
    return gain


def centred(own_key, extent, scale, limit, cuts=(), kind=jnp.bfloat16):
    level = block_levels(own_key, extent, cuts, -0.22, 0.18) if cuts else 1.0
    drawn = jax.random.normal(own_key, extent, jnp.float32) * scale * level
    return jnp.minimum(jnp.maximum(drawn, -limit), limit).astype(kind)


def setup_inputs(seed: int = 0) -> dict:
    arg_keys = jax.random.split(jax.random.key(seed), 14)
    queries = centred(arg_keys[0], (MIXER_TOKENS, RETENTION_HEADS * HEAD_DIM), 1.0, 6.0, ((0, 8), (1, 4)))
    keys = centred(arg_keys[1], (MIXER_TOKENS, RETENTION_HEADS * HEAD_DIM), 1.0, 6.0, ((0, 8), (1, 4)))
    values = centred(arg_keys[2], (MIXER_TOKENS, RETENTION_HEADS * HEAD_DIM), 1.0, 6.0, ((0, 8), (1, 4)))
    gates = centred(arg_keys[3], (MIXER_TOKENS, RETENTION_HEADS * HEAD_DIM), 1.0, 6.0, ((0, 8), (1, 4)))
    log_decay = draw_log_decay(jax.random.fold_in(arg_keys[13], 71), 0)
    out_weight = centred(arg_keys[5], (RETENTION_HEADS * HEAD_DIM, D), (RETENTION_HEADS * HEAD_DIM) ** -0.5, 0.125, ((1, 4),))
    moe_rows = draw_moe_rows(jax.random.fold_in(arg_keys[13], 71), 0)
    moe_gain = jnp.clip(1.0 + 0.18 * jax.random.normal(arg_keys[7], (D,), jnp.float32), 0.099609375, 1.8984375).astype(jnp.bfloat16)
    routes = draw_routes(jax.random.fold_in(arg_keys[13], 71), 0)
    route_weights = jnp.clip(0.1 + 0.9 * jax.random.uniform(arg_keys[9], (TOKENS_MOE, 2), jnp.float32) ** block_levels(arg_keys[9], (TOKENS_MOE, 2), ((0, 8),), -0.2, 0.2), 0.1, 1.0)
    gate_proj = centred(arg_keys[10], (EXPERTS, D, FF), D ** -0.5, 0.125, ((0, 8), (2, 4)))
    up_proj = centred(arg_keys[11], (EXPERTS, D, FF), D ** -0.5, 0.125, ((0, 8), (2, 4)))
    down_proj = centred(arg_keys[12], (EXPERTS, FF, D), FF ** -0.5, 0.09375, ((0, 8), (2, 4)))
    return {"queries": queries, "keys": keys, "values": values, "gates": gates, "log_decay": log_decay, "out_weight": out_weight, "moe_rows": moe_rows, "moe_gain": moe_gain, "routes": routes, "route_weights": route_weights, "gate_proj": gate_proj, "up_proj": up_proj, "down_proj": down_proj}


def rotate(source, factor):
    length = source.shape[0]
    values_f = source.astype(jnp.float32).reshape(length, RETENTION_HEADS, HEAD_DIM)
    half_dim = HEAD_DIM // 2
    inverse = 10000.0 ** (-jnp.arange(half_dim, dtype=jnp.float32) / half_dim)
    angles = jnp.arange(length, dtype=jnp.float32)[:, None] * inverse[None, :]
    cosine = jnp.cos(angles)[:, None, :]
    sine_part = jnp.sin(angles)[:, None, :]
    first_half = values_f[..., :half_dim]
    second_half = values_f[..., half_dim:]
    turned = jnp.concatenate([first_half * cosine - second_half * sine_part, first_half * sine_part + second_half * cosine], axis=-1)
    return (turned * factor).astype(jnp.bfloat16)

def retention_ref(queries, keys, values, gates, log_decay, out_weight):
    length = queries.shape[0]
    block_count = length // BLOCK
    rot_q = rotate(queries, 1.0)
    rot_k = rotate(keys, HEAD_DIM ** (-0.5))
    q_blocks = rot_q.reshape(block_count, BLOCK, RETENTION_HEADS, HEAD_DIM)
    k_blocks = rot_k.reshape(block_count, BLOCK, RETENTION_HEADS, HEAD_DIM)
    v_blocks = values.reshape(block_count, BLOCK, RETENTION_HEADS, HEAD_DIM)
    l_blocks = log_decay.reshape(block_count, BLOCK, RETENTION_HEADS)
    causal = jnp.arange(BLOCK)[:, None] >= jnp.arange(BLOCK)[None, :]

    def advance(carry_state, member):
        q_block, k_block, v_block, l_block = member
        cumulative = jnp.cumsum(l_block, axis=0)
        across = cumulative.T
        spread = across[:, :, None] - across[:, None, :]
        weights = jnp.where(causal, jnp.exp(jnp.where(causal, spread, 0.0)), 0.0)
        q_float = q_block.astype(jnp.float32)
        k_float = k_block.astype(jnp.float32)
        v_float = v_block.astype(jnp.float32)
        scores = jnp.einsum('ihd,jhd->hij', q_float, k_float)
        rounded = lax.optimization_barrier((scores * weights).astype(jnp.bfloat16)).astype(jnp.float32)
        inside = jnp.einsum('hij,jhd->ihd', rounded, v_float)
        carried = jnp.einsum('ihd,hde->ihe', q_float, carry_state, precision=lax.Precision.HIGHEST) * jnp.exp(cumulative)[:, :, None]
        ending = cumulative[-1]
        k_scaled = k_float * jnp.exp(ending[None, :] - cumulative)[:, :, None]
        update = jnp.einsum('jhd,jhe->hde', k_scaled, v_float, precision=lax.Precision.HIGHEST)
        return (jnp.exp(ending)[:, None, None] * carry_state + update, inside + carried)
    zero_state = jnp.zeros((RETENTION_HEADS, HEAD_DIM, HEAD_DIM), jnp.float32)
    _, retained = lax.scan(advance, zero_state, (q_blocks, k_blocks, v_blocks, l_blocks))
    retained = retained.reshape(length, RETENTION_HEADS, HEAD_DIM)
    gate_f = gates.astype(jnp.float32).reshape(length, RETENTION_HEADS, HEAD_DIM)
    scaled = retained * lax.rsqrt(lax.optimization_barrier(jnp.mean(retained * retained, axis=-1, keepdims=True)) + 1e-05)
    head_out = (scaled * jax.nn.silu(gate_f)).astype(jnp.bfloat16).reshape(length, RETENTION_HEADS * HEAD_DIM)
    return jnp.dot(head_out, out_weight, preferred_element_type=jnp.float32).astype(jnp.bfloat16)

def experts_ref(moe_rows, moe_gain, routes, route_weights, gate_proj, up_proj, down_proj):
    as_float = moe_rows.astype(jnp.float32)
    normed = (as_float * lax.rsqrt(lax.optimization_barrier(jnp.mean(as_float * as_float, axis=-1, keepdims=True)) + 1e-06) * moe_gain.astype(jnp.float32)).astype(jnp.bfloat16)
    flat_ids = routes.reshape(-1)
    sorted_slots = jnp.argsort(flat_ids, stable=True).astype(jnp.int32)
    per_expert = flat_ids.shape[0] // EXPERTS
    grouped = normed[sorted_slots // 2].reshape(EXPERTS, per_expert, D)

    def run_expert(member):
        block_rows, w_gate, w_up, w_down = member
        gate_part = jnp.dot(block_rows, w_gate, preferred_element_type=jnp.float32)
        up_part = jnp.dot(block_rows, w_up, preferred_element_type=jnp.float32)
        hidden = (jax.nn.silu(gate_part) * up_part).astype(jnp.bfloat16)
        return jnp.dot(hidden, w_down, preferred_element_type=jnp.float32).astype(jnp.bfloat16)
    outputs = lax.map(run_expert, (grouped, gate_proj, up_proj, down_proj))
    slot_out = jnp.zeros((flat_ids.shape[0], D), jnp.bfloat16).at[sorted_slots].set(outputs.reshape(-1, D))
    weighted = slot_out.astype(jnp.float32).reshape(-1, 2, D) * route_weights[:, :, None]
    return lax.optimization_barrier(jnp.sum(weighted, axis=1)).astype(jnp.bfloat16)

def reference(queries, keys, values, gates, log_decay, out_weight, moe_rows, moe_gain, routes, route_weights, gate_proj, up_proj, down_proj):
    mixer_out = retention_ref(queries, keys, values, gates, log_decay, out_weight)
    moe_out = experts_ref(moe_rows, moe_gain, routes, route_weights, gate_proj, up_proj, down_proj)
    return (mixer_out, moe_out)
```

```python
import functools

import jax
import jax.numpy as jnp
from jax import lax
from jax.experimental import pallas as pl
from jax.experimental.pallas import tpu as pltpu
from jax.sharding import PartitionSpec as P

BLOCK = 128
CHUNKS = 2
MESH = pl.DeviceIdType.MESH
F32 = jnp.float32
BF16 = jnp.bfloat16


def each(low, high, body):
    if high - low <= 8:
        for index in range(low, high):
            body(index)
    else:

        @pl.loop(low, high)
        def _(index):
            body(index)


def span(index, size):
    return pl.ds(pl.multiple_of(index * size, size), size)


def split(value):
    high = value.astype(BF16)
    return high, (value - high.astype(F32)).astype(BF16)


def dot(a, b, dims=((1,), (0,))):
    return lax.dot_general(a, b, (dims, ((), ())), preferred_element_type=F32)


class Gather:
    def __init__(self, tp, region, half, send, recv):
        self.tp, self.region, self.half, self.send, self.recv = tp, region, half, send, recv
        self.me = lax.axis_index("tp")

    def copy(self, ref, slot, to):
        return pltpu.make_async_remote_copy(
            src_ref=ref, dst_ref=ref, send_sem=self.send(slot), recv_sem=self.recv(slot),
            device_id={"tp": to}, device_id_type=MESH,
        )

    def outs(self):
        me, tp = self.me, self.tp
        if tp == 4:
            return [self.copy(self.region(me), k - 1, me ^ k) for k in (1, 2)]
        return [self.copy(self.region(me), k - 1, lax.rem(me + k, tp)) for k in range(1, tp)]

    def hops(self):
        me = self.me
        return [
            self.copy(self.half(me ^ 1, 0), 2, me ^ 2),
            self.copy(self.half(me ^ 2, 1), 3, me ^ 1),
        ]

    def start(self):
        for copy in self.outs():
            copy.start()

    def forward(self):
        if self.tp == 4:
            me = self.me
            hops = self.hops()
            for k in (1, 2):
                self.copy(self.region(me ^ k), k - 1, me ^ k).wait_recv()
                hops[k - 1].start()

    def finish(self):
        me, tp = self.me, self.tp
        if tp == 4:
            self.copy(self.half(me ^ 3, 0), 2, me ^ 2).wait_recv()
            self.copy(self.half(me ^ 3, 1), 3, me ^ 1).wait_recv()
        else:
            for k in range(1, tp):
                owner = lax.rem(me + tp - k, tp)
                self.copy(self.region(owner), k - 1, owner).wait_recv()

    def drain(self):
        for copy in self.outs() + (self.hops() if self.tp == 4 else []):
            copy.wait_send()


def kernel(
    ep, tp,
    q_ref, k_ref, v_ref, g_ref, ld_ref, cos_ref, sin_ref, rows_ref, gain_ref, routes_ref, rw_ref,
    wo_hbm, wg_hbm, wu_hbm, wd_hbm,
    mix_ref, moe_ref,
    wo, wg, wu, wd, normed, p0, p1, og, partner_rows, x, h, eo, ret, ho, state, landed, excl,
    rq, inside, cums,
    w_sem, z_send, z_recv, f_send, f_recv, h_send, h_recv, r_send, r_recv, m_send, m_recv,
    s_send, s_recv,
):
    e, t = lax.axis_index("ep"), lax.axis_index("tp")
    rows, d = rows_ref.shape
    cap = 2 * rows // ep
    dq = d // tp
    ff = wd.shape[0]
    fq = ff // tp
    heads = ld_ref.shape[1]
    hd = q_ref.shape[1] // heads
    blocks = rows // BLOCK
    chunk = ep * cap // CHUNKS
    half_ep = ep // CHUNKS
    pieces = 2 if fq >= 512 else 1
    piece = fq // pieces

    barrier = pltpu.get_barrier_semaphore()

    def greet_ep(off):
        pl.semaphore_signal(barrier, inc=1, device_id={"ep": e ^ off}, device_id_type=MESH)

    each(1, ep, greet_ep)
    for k in range(1, tp):
        pl.semaphore_signal(
            barrier, inc=1, device_id={"tp": lax.rem(t + k, tp)}, device_id_type=MESH
        )

    loads = [
        pltpu.make_async_copy(src, dst, w_sem.at[i])
        for i, (src, dst) in enumerate(
            ((wg_hbm.at[0], wg), (wu_hbm.at[0], wu), (wd_hbm.at[0], wd), (wo_hbm, wo))
        )
    ]
    for load in loads:
        load.start()

    step_rows = 32

    @pl.loop(0, rows // step_rows)
    def _(i):
        at = span(i, step_rows)
        val = rows_ref[at, :].astype(F32)
        scale = lax.rsqrt(jnp.mean(val * val, axis=-1, keepdims=True) + 1e-06)
        normed[at, :] = (val * scale * gain_ref[...].astype(F32)).astype(BF16)

    lanes = lax.broadcasted_iota(jnp.int32, (rows, 128), 1)
    hot = [(routes_ref[:, k : k + 1] == lanes).astype(F32) for k in range(2)]
    before = (
        lax.broadcasted_iota(jnp.int32, (rows, rows), 0)
        > lax.broadcasted_iota(jnp.int32, (rows, rows), 1)
    ).astype(F32).astype(BF16)
    rank = dot(before, (hot[0] + hot[1]).astype(BF16))
    slots = lax.broadcasted_iota(jnp.int32, (rows, ep * cap), 1)
    small = lax.broadcasted_iota(jnp.int32, (rows, cap), 1)
    targets = []
    for k, ref in ((0, p0), (1, p1)):
        target = routes_ref[:, k : k + 1] * cap + jnp.sum(
            rank * hot[k], axis=1, keepdims=True
        ).astype(jnp.int32)
        targets.append(target)
        ref[...] = (slots == target).astype(F32).astype(BF16)
    both = p0[...] + p1[...]
    og[...] = dot(both, normed[:, span(t, dq)], ((0,), (0,))).astype(BF16)

    def block_of(dest):
        base = small + dest * cap
        return ((base == targets[0]) | (base == targets[1])).astype(F32).astype(BF16)

    partner_rows[...] = dot(block_of(e ^ 1), normed[...], ((0,), (0,))).astype(BF16)
    x[span(e, cap), :] = dot(block_of(e), normed[...], ((0,), (0,))).astype(BF16)

    pl.semaphore_wait(barrier, ep - 1 + tp - 1)

    def z_copy(off, here):
        other = e ^ off
        if isinstance(off, int) and off == 1:
            src, dst = partner_rows, x.at[span(other if here else e, cap), :]
        else:
            src = og.at[span(other, cap), :]
            dst = x.at[span(other if here else e, cap), span(t, dq)]
        return pltpu.make_async_remote_copy(
            src_ref=src, dst_ref=dst, send_sem=z_send.at[other],
            recv_sem=z_recv.at[other if here else e],
            device_id={"ep": other}, device_id_type=MESH,
        )

    z_copy(1, False).start()
    each(2, ep, lambda off: z_copy(off, False).start())

    row_i = lax.broadcasted_iota(jnp.int32, (BLOCK, BLOCK), 0)
    col_j = lax.broadcasted_iota(jnp.int32, (BLOCK, BLOCK), 1)
    causal = row_i >= col_j
    lower = causal.astype(F32)
    factor = hd ** (-0.5)
    for b in range(blocks):
        at = slice(b * BLOCK, (b + 1) * BLOCK)
        cums[at, :] = lax.dot_general(
            lower, ld_ref[at, :], (((1,), (0,)), ((), ())),
            preferred_element_type=F32, precision=lax.Precision.HIGHEST,
        )
    decay_at = heads * hd
    for n in range(heads):
        cols = slice(n * hd, (n + 1) * hd)
        total = None
        gone = None
        for b in range(blocks):
            at = slice(b * BLOCK, (b + 1) * BLOCK)
            cos, sin = cos_ref[at, :], sin_ref[at, :]

            def turned(ref):
                val = ref[at, cols].astype(F32)
                return val * cos + pltpu.roll(val, hd // 2, 1) * sin

            qb = turned(q_ref).astype(BF16)
            kb = (turned(k_ref) * factor).astype(BF16)
            vb = v_ref[at, cols]
            rq[at, cols] = qb
            cum = jnp.broadcast_to(cums[at, n : n + 1], (BLOCK, BLOCK))
            spread = cum - cum.T
            weight = jnp.where(causal, jnp.exp(jnp.where(causal, spread, 0.0)), 0.0)
            scores = dot(qb, kb, ((1,), (1,)))
            inside[at, cols] = dot((scores * weight).astype(BF16), vb)
            ending = cum[BLOCK - 1 : BLOCK, :]
            k_hi, k_lo = split(kb.astype(F32) * jnp.exp(ending - cum))
            update = dot(k_hi, vb, ((0,), (0,))) + dot(k_lo, vb, ((0,), (0,)))
            if b == 0:
                total, gone = update, ending
            else:
                if b < blocks:
                    pass
                total = jnp.exp(ending) * total + update
                gone = gone + ending
            if b < blocks - 1:
                excl[1 + b, n * hd : (n + 1) * hd, :] = total
        state[0, n * hd : (n + 1) * hd, :] = total
        state[0, decay_at + n : decay_at + n + 1, :] = jnp.exp(gone)

    excl[0, :decay_at, :] = jnp.zeros((decay_at, hd), F32)
    excl[0, decay_at : decay_at + heads, :] = jnp.ones((heads, hd), F32)

    rounds = state.shape[0]

    def s_copy(r):
        return pltpu.make_async_remote_copy(
            src_ref=state.at[r], dst_ref=landed.at[r], send_sem=s_send.at[r],
            recv_sem=s_recv.at[r], device_id={"ep": lax.rem(e + 2**r, ep)}, device_id_type=MESH,
        )

    def scan_send(r):
        @pl.when(e + 2**r < ep)
        def _():
            s_copy(r).start()

    def scan_take(r):
        last = r == rounds - 1

        @pl.when(e >= 2**r)
        def _():
            s_copy(r).wait_recv()
            for n in range(heads):
                at = slice(n * hd, (n + 1) * hd)
                da = slice(decay_at + n, decay_at + n + 1)
                came, came_d = landed[r, at, :], landed[r, da, :]
                own_d = excl[0, da, :]
                excl[0, at, :] = own_d * came + excl[0, at, :]
                excl[0, da, :] = own_d * came_d
                if not last:
                    mine_d = state[r, da, :]
                    state[r + 1, at, :] = mine_d * came + state[r, at, :]
                    state[r + 1, da, :] = mine_d * came_d

        if not last:

            @pl.when(e < 2**r)
            def _():
                state[r + 1, : decay_at + heads, :] = state[r, : decay_at + heads, :]

    def row_gather(off):
        other = e ^ off
        start = other * cap

        def half(owner, k):
            return x.at[
                pl.ds(pl.multiple_of(start + k * (cap // 2), cap // 2), cap // 2), span(owner, dq)
            ]

        return Gather(
            tp, lambda owner: x.at[span(other, cap), span(owner, dq)], half,
            lambda slot: f_send.at[other, slot], lambda slot: f_recv.at[other, slot],
        )

    def part_of(c):
        return (e // half_ep) ^ c

    def hid_gather(c, j):
        base = part_of(c) * chunk

        def cols(owner):
            return pl.ds(pl.multiple_of(owner * fq + j * piece, piece), piece)

        return Gather(
            tp,
            lambda owner: h.at[pl.ds(pl.multiple_of(base, chunk), chunk), cols(owner)],
            lambda owner, k: h.at[
                pl.ds(pl.multiple_of(base + k * (chunk // 2), chunk // 2), chunk // 2), cols(owner)
            ],
            lambda slot: h_send.at[c * pieces + j, slot],
            lambda slot: h_recv.at[c * pieces + j, slot],
        )

    mix_gather = Gather(
        tp, lambda owner: ho.at[:, span(owner, heads * hd)],
        lambda owner, k: ho.at[k * (rows // 2) : (k + 1) * (rows // 2), span(owner, heads * hd)],
        lambda slot: m_send.at[slot], lambda slot: m_recv.at[slot],
    )

    def take_rows(off):
        z_copy(off, True).wait_recv()
        row_gather(off).start()

    def hidden_piece(c, j):
        at = pl.ds(pl.multiple_of(part_of(c) * chunk, chunk), chunk)
        tile = min(256, piece)

        @pl.loop(0, piece // tile)
        def _(i):
            cols = pl.ds(pl.multiple_of(j * piece + i * tile, tile), tile)
            held = x[at, :]
            gate = dot(held, wg[:, cols])
            up = dot(held, wu[:, cols])
            hid = (gate / (1.0 + jnp.exp(-gate)) * up).astype(BF16)
            h[at, pl.ds(pl.multiple_of(t * fq + j * piece + i * tile, tile), tile)] = hid

        hid_gather(c, j).start()

    def back_copy(off, here):
        other = e ^ off
        return pltpu.make_async_remote_copy(
            src_ref=eo.at[span(other, cap), :], dst_ref=ret.at[span(other if here else e, cap), :],
            send_sem=r_send.at[other], recv_sem=r_recv.at[other if here else e],
            device_id={"ep": other}, device_id_type=MESH,
        )

    def down(c):
        at = pl.ds(pl.multiple_of(part_of(c) * chunk, chunk), chunk)
        tile = min(256, dq)

        @pl.loop(0, dq // tile)
        def _(i):
            cols = pl.ds(pl.multiple_of(i * tile, tile), tile)
            eo[at, cols] = dot(h[at, :], wd[:, cols]).astype(BF16)

        if c == 0:
            ret[span(e, cap), :] = eo[span(e, cap), :]
        each(max(1, c * half_ep), (c + 1) * half_ep, lambda off: back_copy(off, False).start())

    scan_send(0)
    each(2, half_ep, take_rows)
    each(half_ep, ep, take_rows)
    scan_take(0)
    if rounds > 1:
        scan_send(1)
    each(2, half_ep, lambda off: row_gather(off).forward())
    loads[0].wait()
    loads[1].wait()
    z_copy(1, True).wait_recv()
    each(2, half_ep, lambda off: row_gather(off).finish())
    hidden_piece(0, 0)
    each(half_ep, ep, lambda off: row_gather(off).forward())
    for j in range(1, pieces):
        hidden_piece(0, j)
    if rounds > 1:
        scan_take(1)
    if rounds > 2:
        scan_send(2)
    each(half_ep, ep, lambda off: row_gather(off).finish())
    hid_gather(0, 0).forward()
    hidden_piece(1, 0)
    for j in range(1, pieces):
        hid_gather(0, j).forward()
    for j in range(1, pieces):
        hidden_piece(1, j)
    for r in range(2, rounds):
        scan_take(r)
        if r + 1 < rounds:
            scan_send(r + 1)

    for n in range(heads):
        cols = slice(n * hd, (n + 1) * hd)
        sat = slice(n * hd, (n + 1) * hd)
        entering = excl[0, sat, :]
        gone = None
        for b in range(blocks):
            at = slice(b * BLOCK, (b + 1) * BLOCK)
            cum = jnp.broadcast_to(cums[at, n : n + 1], (BLOCK, hd))
            held = entering if b == 0 else jnp.exp(gone) * entering + excl[b, sat, :]
            hi, lo = split(held)
            qb = rq[at, cols]
            retained = inside[at, cols] + (dot(qb, hi) + dot(qb, lo)) * jnp.exp(cum)
            scale = lax.rsqrt(jnp.mean(retained * retained, axis=-1, keepdims=True) + 1e-05)
            gate = g_ref[at, cols].astype(F32)
            out = (retained * scale * (gate / (1.0 + jnp.exp(-gate)))).astype(BF16)
            ho[at, pl.ds(pl.multiple_of(t * heads * hd + n * hd, hd), hd)] = out
            ending = cum[BLOCK - 1 : BLOCK, :]
            gone = ending if gone is None else gone + ending
    mix_gather.start()

    loads[2].wait()
    loads[3].wait()
    for j in range(pieces):
        hid_gather(0, j).finish()
    hid_gather(1, 0).forward()
    down(0)
    for j in range(1, pieces):
        hid_gather(1, j).forward()
    mix_gather.forward()
    for j in range(pieces):
        hid_gather(1, j).finish()
    down(1)
    mix_gather.finish()
    tile = min(256, dq)

    @pl.loop(0, dq // tile)
    def _(i):
        cols = pl.ds(pl.multiple_of(i * tile, tile), tile)
        mix_ref[:, cols] = dot(ho[...], wo[:, cols]).astype(BF16)

    each(1, ep, lambda off: back_copy(off, True).wait_recv())

    @pl.loop(0, dq // tile)
    def _(i):
        cols = pl.ds(pl.multiple_of(i * tile, tile), tile)
        came = ret[:, cols]
        moe_ref[:, cols] = (
            dot(p0[...], came) * rw_ref[:, 0:1] + dot(p1[...], came) * rw_ref[:, 1:2]
        ).astype(BF16)

    z_copy(1, False).wait_send()
    each(2, ep, lambda off: z_copy(off, False).wait_send())
    each(2, ep, lambda off: row_gather(off).drain())
    each(1, ep, lambda off: back_copy(off, False).wait_send())
    for c in range(CHUNKS):
        for j in range(pieces):
            hid_gather(c, j).drain()
    mix_gather.drain()
    for r in range(rounds):

        @pl.when(e + 2**r < ep)
        def _():
            s_copy(r).wait_send()


def on_device(
    ep, tp,
    queries, keys, values, gates, log_decay, out_weight, moe_rows, moe_gain, routes,
    route_weights, gate_proj, up_proj, down_proj,
):
    rows, d = moe_rows.shape
    heads = log_decay.shape[1]
    width = queries.shape[1]
    hd = width // heads
    cap = 2 * rows // ep
    dq = d // tp
    fq = gate_proj.shape[2]
    ff = down_proj.shape[1]
    rounds = (ep - 1).bit_length()
    slots = max(4, tp - 1)
    pieces = CHUNKS * 2
    blocks = rows // BLOCK
    positions = (lax.axis_index("ep") * rows + jnp.arange(rows, dtype=jnp.int32)).astype(F32)
    half = hd // 2
    inverse = 10000.0 ** (-jnp.arange(half, dtype=F32) / half)
    angles = positions[:, None] * jnp.tile(inverse, 2)[None, :]
    sign = jnp.where(jnp.arange(hd) < half, -1.0, 1.0).astype(F32)
    cos, sin = jnp.cos(angles), jnp.sin(angles) * sign[None, :]
    srows = heads * hd + 8 * ((heads + 7) // 8)
    vmem = pl.BlockSpec(memory_space=pltpu.VMEM)
    hbm = pl.BlockSpec(memory_space=pl.ANY)
    dma = pltpu.SemaphoreType.DMA
    out = jax.ShapeDtypeStruct((rows, dq), BF16)
    return pl.pallas_call(
        functools.partial(kernel, ep, tp),
        out_shape=(out, out),
        in_specs=[vmem] * 11 + [hbm] * 4,
        out_specs=(vmem, vmem),
        scratch_shapes=[
            pltpu.VMEM(out_weight.shape, BF16),
            pltpu.VMEM((d, fq), BF16),
            pltpu.VMEM((d, fq), BF16),
            pltpu.VMEM((ff, dq), BF16),
            pltpu.VMEM((rows, d), BF16),
            pltpu.VMEM((rows, ep * cap), BF16),
            pltpu.VMEM((rows, ep * cap), BF16),
            pltpu.VMEM((ep * cap, dq), BF16),
            pltpu.VMEM((cap, d), BF16),
            pltpu.VMEM((ep * cap, d), BF16),
            pltpu.VMEM((ep * cap, ff), BF16),
            pltpu.VMEM((ep * cap, dq), BF16),
            pltpu.VMEM((ep * cap, dq), BF16),
            pltpu.VMEM((rows, width * tp), BF16),
            pltpu.VMEM((rounds, srows, hd), F32),
            pltpu.VMEM((rounds, srows, hd), F32),
            pltpu.VMEM((blocks, srows, hd), F32),
            pltpu.VMEM((rows, width), BF16),
            pltpu.VMEM((rows, width), F32),
            pltpu.VMEM((rows, heads), F32),
            dma((4,)),
            dma((ep,)), dma((ep,)),
            dma((ep, slots)), dma((ep, slots)),
            dma((pieces, slots)), dma((pieces, slots)),
            dma((ep,)), dma((ep,)),
            dma((slots,)), dma((slots,)),
            dma((rounds,)), dma((rounds,)),
        ],
        compiler_params=pltpu.CompilerParams(
            collective_id=0, has_side_effects=True, vmem_limit_bytes=60 * 1024 * 1024
        ),
    )(
        queries, keys, values, gates, log_decay, cos, sin, moe_rows, moe_gain[None, :], routes,
        route_weights, out_weight, gate_proj, up_proj, down_proj,
    )


def solution(mesh):
    placed = (
        P("ep", "tp"), P("ep", "tp"), P("ep", "tp"), P("ep", "tp"), P("ep", "tp"),
        P(None, "tp"), P("ep", None), P(), P("ep", None), P("ep", None),
        P("ep", None, "tp"), P("ep", None, "tp"), P("ep", None, "tp"),
    )
    return jax.shard_map(
        functools.partial(on_device, mesh.shape["ep"], mesh.shape["tp"]),
        mesh=mesh, in_specs=placed, out_specs=(P("ep", "tp"), P("ep", "tp")), check_vma=False,
    )
```

```python
import functools

import jax
import jax.numpy as jnp
from jax import lax
from jax.experimental import pallas as pl
from jax.experimental.pallas import tpu as pltpu
from jax.sharding import PartitionSpec as P

BLOCK = 128
CHUNKS = 2
MESH = pl.DeviceIdType.MESH
F32 = jnp.float32
BF16 = jnp.bfloat16


def each(low, high, body):
    if high - low <= 8:
        for index in range(low, high):
            body(index)
    else:

        @pl.loop(low, high)
        def _(index):
            body(index)


def span(index, size):
    return pl.ds(pl.multiple_of(index * size, size), size)


def split(value):
    high = value.astype(BF16)
    return high, (value - high.astype(F32)).astype(BF16)


def dot(a, b, dims=((1,), (0,))):
    return lax.dot_general(a, b, (dims, ((), ())), preferred_element_type=F32)


class Gather:
    def __init__(self, tp, region, half, send, recv):
        self.tp, self.region, self.half, self.send, self.recv = tp, region, half, send, recv
        self.me = lax.axis_index("tp")

    def copy(self, ref, slot, to):
        return pltpu.make_async_remote_copy(
            src_ref=ref, dst_ref=ref, send_sem=self.send(slot), recv_sem=self.recv(slot),
            device_id={"tp": to}, device_id_type=MESH,
        )

    def outs(self):
        me, tp = self.me, self.tp
        if tp == 4:
            return [self.copy(self.region(me), k - 1, me ^ k) for k in (1, 2)]
        return [self.copy(self.region(me), k - 1, lax.rem(me + k, tp)) for k in range(1, tp)]

    def hops(self):
        me = self.me
        return [
            self.copy(self.half(me ^ 1, 0), 2, me ^ 2),
            self.copy(self.half(me ^ 2, 1), 3, me ^ 1),
        ]

    def start(self):
        for copy in self.outs():
            copy.start()

    def forward(self):
        if self.tp == 4:
            me = self.me
            hops = self.hops()
            for k in (1, 2):
                self.copy(self.region(me ^ k), k - 1, me ^ k).wait_recv()
                hops[k - 1].start()

    def finish(self):
        me, tp = self.me, self.tp
        if tp == 4:
            self.copy(self.half(me ^ 3, 0), 2, me ^ 2).wait_recv()
            self.copy(self.half(me ^ 3, 1), 3, me ^ 1).wait_recv()
        else:
            for k in range(1, tp):
                owner = lax.rem(me + tp - k, tp)
                self.copy(self.region(owner), k - 1, owner).wait_recv()

    def drain(self):
        for copy in self.outs() + (self.hops() if self.tp == 4 else []):
            copy.wait_send()


def kernel(
    ep, tp,
    q_ref, k_ref, v_ref, g_ref, ld_ref, cos_ref, sin_ref, rows_ref, gain_ref, routes_ref, rw_ref,
    wo_hbm, wg_hbm, wu_hbm, wd_hbm,
    mix_ref, moe_ref,
    wo, wg, wu, wd, normed, p0, p1, og, partner_rows, x, h, eo, ret, ho, state, landed, excl,
    rq, inside, cums, pack, narrow,
    w_sem, z_send, z_recv, f_send, f_recv, h_send, h_recv, r_send, r_recv, m_send, m_recv,
    s_send, s_recv,
):
    e, t = lax.axis_index("ep"), lax.axis_index("tp")
    rows, d = rows_ref.shape
    cap = 2 * rows // ep
    dq = d // tp
    ff = wd.shape[0]
    fq = ff // tp
    heads = ld_ref.shape[0]
    hd = q_ref.shape[1] // heads
    blocks = rows // BLOCK
    chunk = ep * cap // CHUNKS
    half_ep = ep // CHUNKS
    pieces = 2 if fq >= 512 else 1
    piece = fq // pieces

    barrier = pltpu.get_barrier_semaphore()

    def greet_ep(off):
        pl.semaphore_signal(barrier, inc=1, device_id={"ep": e ^ off}, device_id_type=MESH)

    each(1, ep, greet_ep)
    for k in range(1, tp):
        pl.semaphore_signal(
            barrier, inc=1, device_id={"tp": lax.rem(t + k, tp)}, device_id_type=MESH
        )

    loads = [
        pltpu.make_async_copy(src, dst, w_sem.at[i])
        for i, (src, dst) in enumerate(
            ((wg_hbm.at[0], wg), (wu_hbm.at[0], wu), (wd_hbm.at[0], wd), (wo_hbm, wo))
        )
    ]
    for load in loads:
        load.start()

    pack[...] = jnp.zeros_like(pack)
    pack[0:2, :] = routes_ref[...].astype(F32)
    pack[2:4, :] = rw_ref[...]
    pack[4 : 4 + heads, :] = ld_ref[...]
    for b in range(rows // 128):
        narrow[b * 128 : (b + 1) * 128, :] = pack[:, b * 128 : (b + 1) * 128].T
    routes = [narrow[:, k : k + 1].astype(jnp.int32) for k in range(2)]

    step_rows = 32

    @pl.loop(0, rows // step_rows)
    def _(i):
        at = span(i, step_rows)
        val = rows_ref[at, :].astype(F32)
        scale = lax.rsqrt(jnp.mean(val * val, axis=-1, keepdims=True) + 1e-06)
        for c in range(d // 128):
            cols = slice(c * 128, (c + 1) * 128)
            normed[at, cols] = (val[:, cols] * scale * gain_ref[c : c + 1, :].astype(F32)).astype(
                BF16
            )

    lanes = lax.broadcasted_iota(jnp.int32, (rows, 128), 1)
    hot = [(routes[k] == lanes).astype(F32) for k in range(2)]
    before = (
        lax.broadcasted_iota(jnp.int32, (rows, rows), 0)
        > lax.broadcasted_iota(jnp.int32, (rows, rows), 1)
    ).astype(F32).astype(BF16)
    rank = dot(before, (hot[0] + hot[1]).astype(BF16))
    slots = lax.broadcasted_iota(jnp.int32, (rows, ep * cap), 1)
    small = lax.broadcasted_iota(jnp.int32, (rows, cap), 1)
    targets = []
    for k, ref in ((0, p0), (1, p1)):
        target = routes[k] * cap + jnp.sum(
            rank * hot[k], axis=1, keepdims=True
        ).astype(jnp.int32)
        targets.append(target)
        ref[...] = (slots == target).astype(F32).astype(BF16)
    both = p0[...] + p1[...]
    og[...] = dot(both, normed[:, span(t, dq)], ((0,), (0,))).astype(BF16)

    def block_of(dest):
        base = small + dest * cap
        return ((base == targets[0]) | (base == targets[1])).astype(F32).astype(BF16)

    partner_rows[...] = dot(block_of(e ^ 1), normed[...], ((0,), (0,))).astype(BF16)
    x[span(e, cap), :] = dot(block_of(e), normed[...], ((0,), (0,))).astype(BF16)

    pl.semaphore_wait(barrier, ep - 1 + tp - 1)

    def z_copy(off, here):
        other = e ^ off
        if isinstance(off, int) and off == 1:
            src, dst = partner_rows, x.at[span(other if here else e, cap), :]
        else:
            src = og.at[span(other, cap), :]
            dst = x.at[span(other if here else e, cap), span(t, dq)]
        return pltpu.make_async_remote_copy(
            src_ref=src, dst_ref=dst, send_sem=z_send.at[other],
            recv_sem=z_recv.at[other if here else e],
            device_id={"ep": other}, device_id_type=MESH,
        )

    z_copy(1, False).start()
    each(2, ep, lambda off: z_copy(off, False).start())

    row_i = lax.broadcasted_iota(jnp.int32, (BLOCK, BLOCK), 0)
    col_j = lax.broadcasted_iota(jnp.int32, (BLOCK, BLOCK), 1)
    causal = row_i >= col_j
    lower = causal.astype(F32)
    factor = hd ** (-0.5)
    for b in range(blocks):
        at = slice(b * BLOCK, (b + 1) * BLOCK)
        cums[at, :] = lax.dot_general(
            lower, narrow[at, :], (((1,), (0,)), ((), ())),
            preferred_element_type=F32, precision=lax.Precision.HIGHEST,
        )
    decay_at = heads * hd
    for n in range(heads):
        cols = slice(n * hd, (n + 1) * hd)
        total = None
        gone = None
        for b in range(blocks):
            at = slice(b * BLOCK, (b + 1) * BLOCK)
            cos, sin = cos_ref[at, :], sin_ref[at, :]

            def turned(ref):
                val = ref[at, cols].astype(F32)
                return val * cos + pltpu.roll(val, hd // 2, 1) * sin

            qb = turned(q_ref).astype(BF16)
            kb = (turned(k_ref) * factor).astype(BF16)
            vb = v_ref[at, cols]
            rq[at, cols] = qb
            cum = jnp.broadcast_to(cums[at, 4 + n : 5 + n], (BLOCK, BLOCK))
            spread = cum - cum.T
            weight = jnp.where(causal, jnp.exp(jnp.where(causal, spread, 0.0)), 0.0)
            scores = dot(qb, kb, ((1,), (1,)))
            inside[at, cols] = dot((scores * weight).astype(BF16), vb)
            ending = cum[BLOCK - 1 : BLOCK, :]
            k_hi, k_lo = split(kb.astype(F32) * jnp.exp(ending - cum))
            update = dot(k_hi, vb, ((0,), (0,))) + dot(k_lo, vb, ((0,), (0,)))
            if b == 0:
                total, gone = update, ending
            else:
                if b < blocks:
                    pass
                total = jnp.exp(ending) * total + update
                gone = gone + ending
            if b < blocks - 1:
                excl[1 + b, n * hd : (n + 1) * hd, :] = total
        state[0, n * hd : (n + 1) * hd, :] = total
        state[0, decay_at + n : decay_at + n + 1, :] = jnp.exp(gone)

    excl[0, :decay_at, :] = jnp.zeros((decay_at, hd), F32)
    excl[0, decay_at : decay_at + heads, :] = jnp.ones((heads, hd), F32)

    rounds = state.shape[0]

    def s_copy(r):
        return pltpu.make_async_remote_copy(
            src_ref=state.at[r], dst_ref=landed.at[r], send_sem=s_send.at[r],
            recv_sem=s_recv.at[r], device_id={"ep": lax.rem(e + 2**r, ep)}, device_id_type=MESH,
        )

    def scan_send(r):
        @pl.when(e + 2**r < ep)
        def _():
            s_copy(r).start()

    def scan_take(r):
        last = r == rounds - 1

        @pl.when(e >= 2**r)
        def _():
            s_copy(r).wait_recv()
            for n in range(heads):
                at = slice(n * hd, (n + 1) * hd)
                da = slice(decay_at + n, decay_at + n + 1)
                came, came_d = landed[r, at, :], landed[r, da, :]
                own_d = excl[0, da, :]
                excl[0, at, :] = own_d * came + excl[0, at, :]
                excl[0, da, :] = own_d * came_d
                if not last:
                    mine_d = state[r, da, :]
                    state[r + 1, at, :] = mine_d * came + state[r, at, :]
                    state[r + 1, da, :] = mine_d * came_d

        if not last:

            @pl.when(e < 2**r)
            def _():
                state[r + 1, : decay_at + heads, :] = state[r, : decay_at + heads, :]

    def row_gather(off):
        other = e ^ off
        start = other * cap

        def half(owner, k):
            return x.at[
                pl.ds(pl.multiple_of(start + k * (cap // 2), cap // 2), cap // 2), span(owner, dq)
            ]

        return Gather(
            tp, lambda owner: x.at[span(other, cap), span(owner, dq)], half,
            lambda slot: f_send.at[other, slot], lambda slot: f_recv.at[other, slot],
        )

    def part_of(c):
        return (e // half_ep) ^ c

    def hid_gather(c, j):
        base = part_of(c) * chunk

        def cols(owner):
            return pl.ds(pl.multiple_of(owner * fq + j * piece, piece), piece)

        return Gather(
            tp,
            lambda owner: h.at[pl.ds(pl.multiple_of(base, chunk), chunk), cols(owner)],
            lambda owner, k: h.at[
                pl.ds(pl.multiple_of(base + k * (chunk // 2), chunk // 2), chunk // 2), cols(owner)
            ],
            lambda slot: h_send.at[c * pieces + j, slot],
            lambda slot: h_recv.at[c * pieces + j, slot],
        )

    mix_gather = Gather(
        tp, lambda owner: ho.at[:, span(owner, heads * hd)],
        lambda owner, k: ho.at[k * (rows // 2) : (k + 1) * (rows // 2), span(owner, heads * hd)],
        lambda slot: m_send.at[slot], lambda slot: m_recv.at[slot],
    )

    def take_rows(off):
        z_copy(off, True).wait_recv()
        row_gather(off).start()

    def hidden_piece(c, j):
        at = pl.ds(pl.multiple_of(part_of(c) * chunk, chunk), chunk)
        tile = min(256, piece)

        @pl.loop(0, piece // tile)
        def _(i):
            cols = pl.ds(pl.multiple_of(j * piece + i * tile, tile), tile)
            held = x[at, :]
            gate = dot(held, wg[:, cols])
            up = dot(held, wu[:, cols])
            hid = (gate / (1.0 + jnp.exp(-gate)) * up).astype(BF16)
            h[at, pl.ds(pl.multiple_of(t * fq + j * piece + i * tile, tile), tile)] = hid

        hid_gather(c, j).start()

    def back_copy(off, here):
        other = e ^ off
        return pltpu.make_async_remote_copy(
            src_ref=eo.at[span(other, cap), :], dst_ref=ret.at[span(other if here else e, cap), :],
            send_sem=r_send.at[other], recv_sem=r_recv.at[other if here else e],
            device_id={"ep": other}, device_id_type=MESH,
        )

    def down(c):
        at = pl.ds(pl.multiple_of(part_of(c) * chunk, chunk), chunk)
        tile = min(256, dq)

        @pl.loop(0, dq // tile)
        def _(i):
            cols = pl.ds(pl.multiple_of(i * tile, tile), tile)
            eo[at, cols] = dot(h[at, :], wd[:, cols]).astype(BF16)

        if c == 0:
            ret[span(e, cap), :] = eo[span(e, cap), :]
        each(max(1, c * half_ep), (c + 1) * half_ep, lambda off: back_copy(off, False).start())

    scan_send(0)
    each(2, half_ep, take_rows)
    each(half_ep, ep, take_rows)
    scan_take(0)
    if rounds > 1:
        scan_send(1)
    each(2, half_ep, lambda off: row_gather(off).forward())
    loads[0].wait()
    loads[1].wait()
    z_copy(1, True).wait_recv()
    each(2, half_ep, lambda off: row_gather(off).finish())
    hidden_piece(0, 0)
    each(half_ep, ep, lambda off: row_gather(off).forward())
    for j in range(1, pieces):
        hidden_piece(0, j)
    if rounds > 1:
        scan_take(1)
    if rounds > 2:
        scan_send(2)
    each(half_ep, ep, lambda off: row_gather(off).finish())
    hid_gather(0, 0).forward()
    hidden_piece(1, 0)
    for j in range(1, pieces):
        hid_gather(0, j).forward()
    for j in range(1, pieces):
        hidden_piece(1, j)
    for r in range(2, rounds):
        scan_take(r)
        if r + 1 < rounds:
            scan_send(r + 1)

    for n in range(heads):
        cols = slice(n * hd, (n + 1) * hd)
        sat = slice(n * hd, (n + 1) * hd)
        entering = excl[0, sat, :]
        gone = None
        for b in range(blocks):
            at = slice(b * BLOCK, (b + 1) * BLOCK)
            cum = jnp.broadcast_to(cums[at, 4 + n : 5 + n], (BLOCK, hd))
            held = entering if b == 0 else jnp.exp(gone) * entering + excl[b, sat, :]
            hi, lo = split(held)
            qb = rq[at, cols]
            retained = inside[at, cols] + (dot(qb, hi) + dot(qb, lo)) * jnp.exp(cum)
            scale = lax.rsqrt(jnp.mean(retained * retained, axis=-1, keepdims=True) + 1e-05)
            gate = g_ref[at, cols].astype(F32)
            out = (retained * scale * (gate / (1.0 + jnp.exp(-gate)))).astype(BF16)
            ho[at, pl.ds(pl.multiple_of(t * heads * hd + n * hd, hd), hd)] = out
            ending = cum[BLOCK - 1 : BLOCK, :]
            gone = ending if gone is None else gone + ending
    mix_gather.start()

    loads[2].wait()
    loads[3].wait()
    for j in range(pieces):
        hid_gather(0, j).finish()
    hid_gather(1, 0).forward()
    down(0)
    for j in range(1, pieces):
        hid_gather(1, j).forward()
    mix_gather.forward()
    for j in range(pieces):
        hid_gather(1, j).finish()
    down(1)
    mix_gather.finish()
    tile = min(256, dq)

    @pl.loop(0, dq // tile)
    def _(i):
        cols = pl.ds(pl.multiple_of(i * tile, tile), tile)
        mix_ref[:, cols] = dot(ho[...], wo[:, cols]).astype(BF16)

    each(1, ep, lambda off: back_copy(off, True).wait_recv())

    @pl.loop(0, dq // tile)
    def _(i):
        cols = pl.ds(pl.multiple_of(i * tile, tile), tile)
        came = ret[:, cols]
        moe_ref[:, cols] = (
            dot(p0[...], came) * narrow[:, 2:3] + dot(p1[...], came) * narrow[:, 3:4]
        ).astype(BF16)

    z_copy(1, False).wait_send()
    each(2, ep, lambda off: z_copy(off, False).wait_send())
    each(2, ep, lambda off: row_gather(off).drain())
    each(1, ep, lambda off: back_copy(off, False).wait_send())
    for c in range(CHUNKS):
        for j in range(pieces):
            hid_gather(c, j).drain()
    mix_gather.drain()
    for r in range(rounds):

        @pl.when(e + 2**r < ep)
        def _():
            s_copy(r).wait_send()


def on_device(
    ep, tp,
    queries, keys, values, gates, log_decay, out_weight, moe_rows, moe_gain, routes,
    route_weights, gate_proj, up_proj, down_proj,
):
    rows, d = moe_rows.shape
    heads = log_decay.shape[1]
    width = queries.shape[1]
    hd = width // heads
    cap = 2 * rows // ep
    dq = d // tp
    fq = gate_proj.shape[2]
    ff = down_proj.shape[1]
    rounds = (ep - 1).bit_length()
    slots = max(4, tp - 1)
    pieces = CHUNKS * 2
    blocks = rows // BLOCK
    positions = (lax.axis_index("ep") * rows + jnp.arange(rows, dtype=jnp.int32)).astype(F32)
    half = hd // 2
    inverse = 10000.0 ** (-jnp.arange(half, dtype=F32) / half)
    angles = positions[:, None] * jnp.tile(inverse, 2)[None, :]
    sign = jnp.where(jnp.arange(hd) < half, -1.0, 1.0).astype(F32)
    cos, sin = jnp.cos(angles), jnp.sin(angles) * sign[None, :]
    srows = heads * hd + 8 * ((heads + 7) // 8)
    vmem = pl.BlockSpec(memory_space=pltpu.VMEM)
    hbm = pl.BlockSpec(memory_space=pl.ANY)
    dma = pltpu.SemaphoreType.DMA
    out = jax.ShapeDtypeStruct((rows, dq), BF16)
    return pl.pallas_call(
        functools.partial(kernel, ep, tp),
        out_shape=(out, out),
        in_specs=[vmem] * 11 + [hbm] * 4,
        out_specs=(vmem, vmem),
        scratch_shapes=[
            pltpu.VMEM(out_weight.shape, BF16),
            pltpu.VMEM((d, fq), BF16),
            pltpu.VMEM((d, fq), BF16),
            pltpu.VMEM((ff, dq), BF16),
            pltpu.VMEM((rows, d), BF16),
            pltpu.VMEM((rows, ep * cap), BF16),
            pltpu.VMEM((rows, ep * cap), BF16),
            pltpu.VMEM((ep * cap, dq), BF16),
            pltpu.VMEM((cap, d), BF16),
            pltpu.VMEM((ep * cap, d), BF16),
            pltpu.VMEM((ep * cap, ff), BF16),
            pltpu.VMEM((ep * cap, dq), BF16),
            pltpu.VMEM((ep * cap, dq), BF16),
            pltpu.VMEM((rows, width * tp), BF16),
            pltpu.VMEM((rounds, srows, hd), F32),
            pltpu.VMEM((rounds, srows, hd), F32),
            pltpu.VMEM((blocks, srows, hd), F32),
            pltpu.VMEM((rows, width), BF16),
            pltpu.VMEM((rows, width), F32),
            pltpu.VMEM((rows, 128), F32),
            pltpu.VMEM((128, rows), F32),
            pltpu.VMEM((rows, 128), F32),
            dma((4,)),
            dma((ep,)), dma((ep,)),
            dma((ep, slots)), dma((ep, slots)),
            dma((pieces, slots)), dma((pieces, slots)),
            dma((ep,)), dma((ep,)),
            dma((slots,)), dma((slots,)),
            dma((rounds,)), dma((rounds,)),
        ],
        compiler_params=pltpu.CompilerParams(
            collective_id=0, has_side_effects=True, vmem_limit_bytes=60 * 1024 * 1024
        ),
    )(
        queries, keys, values, gates, log_decay.T, cos, sin, moe_rows, moe_gain.reshape(-1, 128),
        routes.T, route_weights.T, out_weight, gate_proj, up_proj, down_proj,
    )


def solution(mesh):
    placed = (
        P("ep", "tp"), P("ep", "tp"), P("ep", "tp"), P("ep", "tp"), P("ep", "tp"),
        P(None, "tp"), P("ep", None), P(), P("ep", None), P("ep", None),
        P("ep", None, "tp"), P("ep", None, "tp"), P("ep", None, "tp"),
    )
    return jax.shard_map(
        functools.partial(on_device, mesh.shape["ep"], mesh.shape["tp"]),
        mesh=mesh, in_specs=placed, out_specs=(P("ep", "tp"), P("ep", "tp")), check_vma=False,
    )
```
